512 devices in a mesh: dp: 4 (over x), kv: 64 (over z, y), tp: 2 (over core).
Axes of the slice: x: 4, y: 8, z: 8, core: 2. Of those that a mesh axis runs over, the one named last changes fastest.
Arguments:
- tokens: bfloat16 [16, 4096], P('dp', ('kv', 'tp')), may hold values from -11 to 11
- attn_gain: float32 [4096], replicated, may hold values from 0.1 to 1.9
- query_weight: bfloat16 [4096, 4096], P('kv', 'tp'), may hold values from -0.09375 to 0.09375
- key_cache: bfloat16 [16, 16384, 2, 128], P('dp', 'kv', 'tp'), may hold values from -820 to 820
- value_cache: bfloat16 [16, 16384, 2, 128], P('dp', 'kv', 'tp'), may hold values from -6 to 6
- head_lambda: float32 [32], P('tp'), may hold values from 0.3 to 0.8
- head_gain: float32 [128], replicated, may hold values from 0.1 to 1.9
- out_weight: bfloat16 [4096, 4096], P('kv', 'tp'), may hold values from -0.09375 to 0.09375
- mlp_gain: float32 [4096], replicated, may hold values from 0.1 to 1.9
- gate_weight: bfloat16 [11264, 4096], P(('kv', 'tp')), may hold values from -0.09375 to 0.09375
- up_weight: bfloat16 [11264, 4096], P(('kv', 'tp')), may hold values from -0.09375 to 0.09375
- down_weight: bfloat16 [11264, 4096], P(('kv', 'tp')), may hold values from -0.21875 to 0.21875
Outputs:
- mixed: bfloat16 [16, 4096], P('dp', ('kv', 'tp'))
The draws below stay inside these ranges and needn't reach their ends.
All inputs are finite; a program needn't handle non-finite values.
Results may differ from the reference program's by a relative error of at most 0.02.
The reference program's roundings to bfloat16 on the way (of `scaled`, `rotated`, `probs`, `head_out`, `normed` and `hidden`) count: a program that leaves them out, or rounds other values in their place, can miss the bound.
Values may be sent and summed in bfloat16 or wider, within the bound.
A program may use at most 64 MiB of HBM per device.

```python
import jax
import jax.numpy as jnp
from jax import lax

D = 4096
HEADS = 32
KV_HEADS = 2
HEAD = 64
FF = 11264
VALUE = 128
GROUP = 16
BATCH = 16
CACHE_LEN = 16384
N_TP = 2


def draw_tokens(key, part):
    column_scale = 10.0 ** (jnp.arange(D, dtype=jnp.float32) / D - 0.5)
    row_scale = 10.0 ** (jax.random.uniform(jax.random.fold_in(key, 21), (BATCH, 1), jnp.float32) - 0.5)
    base = jnp.clip(jax.random.normal(jax.random.fold_in(key, 24), (BATCH, D), jnp.float32), -4.0, 4.0)
    return (0.25 * row_scale * column_scale * base).astype(jnp.bfloat16)


def draw_key_cache(key, part):
    shape = (BATCH, CACHE_LEN, KV_HEADS, 2 * HEAD)
    base = jnp.clip(jax.random.normal(jax.random.fold_in(key, 11), shape, jnp.float32), -4.0, 4.0)
    spots = jax.random.randint(jax.random.fold_in(key, 12), (BATCH, 1, KV_HEADS, 4), 0, CACHE_LEN - 1)
    strength = jax.random.uniform(jax.random.fold_in(key, 13), (BATCH, 1, KV_HEADS, 4), jnp.float32, 100.0, 200.0)
    flips = jax.random.randint(jax.random.fold_in(key, 14), (BATCH, 1, KV_HEADS, 4), 0, 2)
    signed = strength * (2.0 * flips.astype(jnp.float32) - 1.0)
    place = jnp.arange(CACHE_LEN, dtype=jnp.int32).reshape(1, CACHE_LEN, 1, 1)
    hits = place == spots
    factor = jnp.sum(jnp.where(hits, signed, 0.0), axis=-1, keepdims=True)
    marked = jnp.any(hits, axis=-1, keepdims=True)
    follow_factor = jnp.roll(factor, 1, axis=1)
    follow = jnp.logical_and(jnp.roll(marked, 1, axis=1), jnp.logical_not(marked))
    lifted = jnp.roll(base, 1, axis=1)
    planted = jnp.where(marked, factor * base, jnp.where(follow, 1.01 * follow_factor * lifted, 2.0 * base))
    return planted.astype(jnp.bfloat16)


def spiked(array, stream_key, source, target, blocks, factor):
    def block_of(dim):
        return (jnp.arange(array.shape[dim]) // (array.shape[dim] // blocks)).reshape((-1,) + (1,) * (array.ndim - 1 - dim))

    one_side = jax.random.permutation(stream_key, blocks)[block_of(target)]
    second = (block_of(target) + blocks // 2) % blocks
    return jnp.where((block_of(source) == one_side) | (block_of(source) == second), factor * array, array)


def levels(stream_key, dims, split, least, high):
    loudness, own = 1.0, jax.random.fold_in(stream_key, 6)
    for axis_at, blocks in split:
        steps = jnp.exp(jax.random.uniform(jax.random.fold_in(own, axis_at), (blocks,), jnp.float32, least / len(split), high / len(split)))
        loudness = loudness * jnp.repeat(steps, dims[axis_at] // blocks).reshape([-1 if axis == axis_at else 1 for axis in range(len(dims))])
    return loudness


def gaussian(own_key, dims, scale, most, cuts=(), kind=jnp.bfloat16):
    result = scale * jax.random.normal(own_key, dims, jnp.float32)
    if cuts:
        result = result * levels(own_key, dims, cuts, -0.22, 0.18)
    return jnp.clip(result, -most, most).astype(kind)


def gaussian_with(stream_key, dims, deviation, limit, pieces, heavy, kind=jnp.bfloat16):
    values = deviation * jax.random.normal(stream_key, dims, jnp.float32)
    if pieces:
        values = values * levels(stream_key, dims, pieces, -0.22, 0.18)
    return jnp.clip(spiked(values, jax.random.fold_in(stream_key, 3), *heavy), -limit, limit).astype(kind)


def setup_inputs(seed: int = 0) -> dict:
    key_of = jax.random.split(jax.random.key(seed), 13)
    return {
        "tokens": draw_tokens(jax.random.fold_in(key_of[12], 71), 0),
        "attn_gain": jnp.clip(1.0 + 0.18 * jax.random.normal(key_of[1], (D,), jnp.float32), 0.1, 1.9),
        "query_weight": gaussian(key_of[2], (D, HEADS * 2 * HEAD), D ** -0.5, 0.09375, ((0, 64), (1, 2))),
        "key_cache": draw_key_cache(jax.random.fold_in(key_of[12], 71), 0),
        "value_cache": gaussian(key_of[4], (BATCH, CACHE_LEN, KV_HEADS, VALUE), 1.0, 6.0, ((0, 4), (1, 64), (2, 2))),
        "head_lambda": jnp.clip(0.3 + 0.5 * jax.random.uniform(key_of[5], (HEADS,), jnp.float32) ** levels(key_of[5], (HEADS,), ((0, 2),), -0.2, 0.2), 0.3, 0.8),
        "head_gain": jnp.clip(1.0 + 0.18 * jax.random.normal(key_of[6], (VALUE,), jnp.float32), 0.1, 1.9),
        "out_weight": gaussian(key_of[7], (D, HEADS * VALUE), (HEADS * VALUE) ** -0.5, 0.09375, ((0, 64), (1, 2))),
        "mlp_gain": jnp.clip(1.0 + 0.18 * jax.random.normal(key_of[8], (D,), jnp.float32), 0.1, 1.9),
        "gate_weight": gaussian(key_of[9], (FF, D), D ** -0.5, 0.09375, ((0, 128),)),
        "up_weight": gaussian(key_of[10], (FF, D), D ** -0.5, 0.09375, ((0, 128),)),
        "down_weight": gaussian_with(key_of[11], (FF, D), FF ** -0.5, 0.21875, ((0, 128),), (0, 1, 128, 5.5)),
    }


EPS = 1e-06
THETA = 10000.0

def rotate(vector, position):
    half_len = vector.shape[-1] // 2
    inv_freq = 1.0 / THETA ** (jnp.arange(half_len, dtype=jnp.float32) / half_len)
    angles = position * inv_freq
    cos_table = jnp.cos(angles)
    sin_table = jnp.sin(angles)
    first_half = vector[..., :half_len]
    second_half = vector[..., half_len:]
    return jnp.concatenate([first_half * cos_table - second_half * sin_table, second_half * cos_table + first_half * sin_table], axis=-1)

def reference(tokens, attn_gain, query_weight, key_cache, value_cache, head_lambda, head_gain, out_weight, mlp_gain, gate_weight, up_weight, down_weight):
    as_float = tokens.astype(jnp.float32)
    mean_square = lax.optimization_barrier(jnp.mean(as_float * as_float, axis=-1, keepdims=True))
    scaled = (as_float * attn_gain).astype(jnp.bfloat16)
    queries = jnp.dot(scaled, query_weight, preferred_element_type=jnp.float32) * lax.rsqrt(mean_square + EPS)
    queries = queries.reshape(BATCH, HEADS, 2, HEAD)
    rotated = rotate(queries, jnp.float32(CACHE_LEN)).astype(jnp.bfloat16)
    lam_grid = head_lambda.reshape(KV_HEADS, GROUP, 1)

    def attend(item):
        query_row, key_rows, value_rows = item
        query_grid = query_row.reshape(KV_HEADS, GROUP, 2, HEAD).astype(jnp.float32)
        key_grid = key_rows.reshape(CACHE_LEN, KV_HEADS, 2, HEAD).astype(jnp.float32)
        scores = jnp.einsum('kgch,lkch->kgcl', query_grid, key_grid) * HEAD ** (-0.5)
        top_score = lax.optimization_barrier(jnp.max(scores, axis=-1, keepdims=True))
        weights_exp = jnp.exp(scores - top_score)
        exp_total = lax.optimization_barrier(jnp.sum(weights_exp, axis=-1))
        probs = weights_exp.astype(jnp.bfloat16).astype(jnp.float32)
        weighted = jnp.einsum('kgcl,lkv->kgcv', probs, value_rows.astype(jnp.float32))
        attended = weighted / exp_total[..., None]
        difference = attended[:, :, 0] - lam_grid * attended[:, :, 1]
        head_norm = lax.rsqrt(lax.optimization_barrier(jnp.mean(difference * difference, axis=-1, keepdims=True)) + EPS)
        head_out = difference * head_norm * head_gain
        return head_out.reshape(HEADS * VALUE).astype(jnp.bfloat16)
    head_out = lax.map(attend, (rotated, key_cache, value_cache))
    group_rows = HEADS * VALUE // N_TP
    attention = jnp.zeros((BATCH, D), jnp.float32)
    for tp_slot in range(N_TP):
        block_out = lax.dot_general(head_out[:, tp_slot * group_rows:(tp_slot + 1) * group_rows], out_weight[:, tp_slot * group_rows:(tp_slot + 1) * group_rows], (((1,), (1,)), ((), ())), preferred_element_type=jnp.float32).astype(jnp.bfloat16)
        attention = attention + block_out.astype(jnp.float32)
    stream = as_float + attention
    stream_square = lax.optimization_barrier(jnp.mean(stream * stream, axis=-1, keepdims=True))
    normed = (stream * lax.rsqrt(stream_square + EPS) * mlp_gain).astype(jnp.bfloat16)
    gate_out = lax.dot_general(normed, gate_weight, (((1,), (1,)), ((), ())), preferred_element_type=jnp.float32)
    up_out = lax.dot_general(normed, up_weight, (((1,), (1,)), ((), ())), preferred_element_type=jnp.float32)
    hidden = (jax.nn.silu(gate_out) * up_out).astype(jnp.bfloat16)
    down_out = jnp.dot(hidden, down_weight, preferred_element_type=jnp.float32)
    return (stream + down_out).astype(jnp.bfloat16)
```

```python
import functools

import jax
import jax.numpy as jnp
import numpy as np
from jax import lax
from jax.experimental import pallas as pl
from jax.experimental.pallas import tpu as pltpu
from jax.sharding import Mesh
from jax.sharding import PartitionSpec as P

KV = ("kv_0", "kv_1")
KV_TP = ("kv_0", "kv_1", "tp")
AXES = ("dp", "kv_0", "kv_1", "tp")
MESH = pl.DeviceIdType.MESH
EPS = 1e-06
THETA = 10000.0
F32 = jnp.float32
BF16 = jnp.bfloat16
N = 8
FAR_FIRST = (4, 3, 5, 2, 6, 1, 7, 0)
RING = FAR_FIRST[:7]
PLANE = [(a, b) for a in FAR_FIRST for b in FAR_FIRST if a or b]
OTHERS = [(a, b, c) for a in FAR_FIRST for b in FAR_FIRST for c in (1, 0) if a or b or c]


def iota(shape, dim):
    return lax.broadcasted_iota(jnp.int32, shape, dim)


def contract_last(left, right):
    return lax.dot_general(left, right, (((1,), (1,)), ((), ())), preferred_element_type=F32)


def rounded(x):
    return x.astype(BF16).astype(F32)


def kernel(
    tok_h, ag_h, wq_h, k_h, v_h, lam_h, hg_h, wo_h, mg_h, wg_h, wu_h, wd_h, rope_h,
    out_ref,
    tok, ag, wq, kc, vc, lam, hg, wo, mg, wg, wu, wd, rope,
    tokx, wox, qs, qr, qz, qzr, qa, ss, sr, hb, sf, gs, gr, gf, qp,
    lsem, psem, ssem, rsem,
):
    d, z, y, t = (lax.axis_index(a) for a in AXES)
    kv = z * N + y
    dev = kv * 2 + t
    owned = y * N + z

    def at(dz, dy, dt):
        return (d, lax.rem(z + dz, N), lax.rem(y + dy, N), lax.rem(t + dt, 2))

    barrier = pltpu.get_barrier_semaphore()
    near = [(0, k, 0) for k in RING] + [(k, 0, 0) for k in RING] + [(0, 0, 1)]
    for p in near:
        pl.semaphore_signal(barrier, inc=1, device_id=at(*p), device_id_type=MESH)

    pairs = (
        (tok_h, tok), (ag_h, ag), (wq_h, wq), (mg_h, mg), (rope_h, rope), (wo_h, wo), (k_h, kc),
        (v_h, vc), (lam_h, lam), (hg_h, hg), (wg_h, wg), (wu_h, wu), (wd_h, wd),
    )
    loads = {}
    for k, (src, dst) in enumerate(pairs):
        loads[k] = pltpu.make_async_copy(src, dst, lsem.at[k])
        loads[k].start()

    def remote(src, dst, k, p):
        return pltpu.make_async_remote_copy(
            src_ref=src, dst_ref=dst, send_sem=ssem.at[k], recv_sem=rsem.at[k],
            device_id=at(*p), device_id_type=MESH,
        )

    row8 = iota((8, 128), 0)
    lane8 = iota((8, 128), 1)

    loads[0].wait()
    loads[1].wait()
    loads[2].wait()
    gain_row = jnp.broadcast_to(ag[pl.ds(dev // 4, 1), :], (8, 128))

    def gain_of(index):
        return pltpu.roll(gain_row, lax.rem(128 - 32 * lax.rem(index, 4), 128), 1)[:, :32]

    def twice(x):
        wide = x.astype(F32)
        return jnp.concatenate([wide, wide], axis=0)

    own8 = twice(tok[...])
    half = pl.multiple_of(t * 32, 32)
    rest = pl.multiple_of((1 - t) * 32, 32)
    qp[...] = jnp.dot((own8 * gain_of(dev)).astype(BF16), wq[pl.ds(half, 32), :], preferred_element_type=F32)
    own_square = jnp.sum(own8 * own8, axis=1, keepdims=True)
    other_gain = gain_of(dev + 1 - 2 * t)

    loads[3].wait()
    for v in range(16):
        two = jnp.where(row8 < 4, mg[2 * v : 2 * v + 1, :], mg[2 * v + 1 : 2 * v + 2, :])
        kept = jnp.where(lane8 // 32 == row8 % 4, two, 0.0)
        full = kept + pltpu.roll(kept, 32, 1)
        gf[8 * v : 8 * v + 8, :] = full + pltpu.roll(full, 64, 1)

    pl.semaphore_wait(barrier, len(near))

    remote(tok, tokx, 0, (0, 0, 1)).start()
    remote(tok, tokx, 0, (0, 0, 1)).wait_recv()
    other8 = twice(tokx[...])
    queries = qp[...] + jnp.dot(
        (other8 * other_gain).astype(BF16), wq[pl.ds(rest, 32), :], preferred_element_type=F32
    )
    square = jnp.broadcast_to(
        own_square + jnp.sum(other8 * other8, axis=1, keepdims=True), (8, 128)
    )
    for j in range(N):
        left = queries[:, 256 * j : 256 * j + 128]
        right = queries[:, 256 * j + 128 : 256 * j + 256]
        qs[j, 0:8, :] = jnp.where(row8 < 4, left, right)
        qs[j, 8:16, :] = square
    for k in RING:
        remote(qs.at[lax.rem(y + k, N)], qr.at[k - 1], 1, (0, k, 0)).start()

    loads[5].wait()
    remote(wo.at[pl.ds(rest, 32), :], wox, 2, (0, 0, 1)).start()

    remote(qr, qr, 1, (0, 1, 0)).wait_recv()
    qz[...] = jnp.sum(qr[...], axis=0) + qs[y]
    for k in RING:
        remote(qz, qzr.at[k - 1], 3, (k, 0, 0)).start()
    loads[4].wait()
    remote(qzr, qzr, 3, (1, 0, 0)).wait_recv()
    total = jnp.sum(qzr[...], axis=0) + qz[...]
    mean_square = total[8:16] * (1.0 / 4096.0)
    query = total[0:8] * lax.rsqrt(mean_square + EPS)
    swapped = jnp.where(lane8 % 64 < 32, pltpu.roll(query, 96, 1), pltpu.roll(query, 32, 1))
    qa[y] = rounded(query * rope[0] + swapped * rope[1])
    for k in RING:
        remote(qa.at[y], qa.at[y], 4, (0, k, 0)).start()
    loads[6].wait()
    loads[7].wait()
    remote(qa.at[0:7], qa.at[0:7], 4, (0, 1, 0)).wait_recv()

    rotated = qa[...].reshape(64, 128)
    low = iota((64, 128), 1) < 64
    both = jnp.concatenate(
        [jnp.where(low, rotated, 0.0), jnp.where(low, 0.0, rotated)], axis=0
    ).astype(BF16)
    sequence = iota((128, 256), 0) % 4
    scores = contract_last(both, kc[0])
    for b in range(1, 4):
        scores = jnp.where(sequence == b, contract_last(both, kc[b]), scores)
    scores = scores * 0.125
    peak = jnp.max(scores, axis=1, keepdims=True)
    raised = jnp.exp(scores - peak)
    mass = jnp.sum(raised, axis=1, keepdims=True)
    probs = raised.astype(BF16)
    sequence_v = iota((128, 128), 0) % 4
    weighted = jnp.dot(probs, vc[0], preferred_element_type=F32)
    for b in range(1, 4):
        weighted = jnp.where(
            sequence_v == b, jnp.dot(probs, vc[b], preferred_element_type=F32), weighted
        )
    lane64 = iota((64, 128), 1)
    ss[0] = weighted[:64]
    ss[1] = weighted[64:]
    ss[2] = jnp.where(
        lane64 == 0, peak[:64],
        jnp.where(lane64 == 1, peak[64:], jnp.where(lane64 == 2, mass[:64], mass[64:])),
    )
    for p in PLANE:
        to = lax.rem(y + p[1], N) * N + lax.rem(z + p[0], N)
        remote(ss.at[:, pl.ds(to, 1), :], sr.at[:, pl.ds(owned, 1), :], 5, (*p, 0)).start()
    for k in range(3):
        sr[k, pl.ds(owned, 1), :] = ss[k, pl.ds(owned, 1), :]
    loads[8].wait()
    loads[9].wait()
    remote(ss.at[:, 0:63, :], sr.at[:, 0:63, :], 5, (0, 1, 0)).wait_recv()

    marks = sr[2]

    def attended(c):
        peaks = marks[:, c : c + 1]
        factor = jnp.exp(peaks - jnp.max(peaks, axis=0, keepdims=True))
        whole = jnp.sum(marks[:, c + 2 : c + 3] * factor, axis=0, keepdims=True)
        return jnp.sum(sr[c] * factor, axis=0, keepdims=True) / whole

    head = 2 * y + z // 4
    difference = attended(0) - lam[head] * attended(1)
    head_norm = lax.rsqrt(jnp.mean(difference * difference, axis=1, keepdims=True) + EPS)
    hb[t, pl.ds(owned, 1), :] = rounded(difference * head_norm * hg[...])
    spot = hb.at[t, pl.ds(owned, 1), :]
    for p in OTHERS:
        remote(spot, spot, 6, p).start()
    remote(wox, wox, 2, (0, 0, 1)).wait_recv()
    remote(sf.at[0:127], sf.at[0:127], 6, (0, 1, 0)).wait_recv()

    def projected(group, weight):
        heads = hb[group]
        tiles = []
        for j in range(N):
            tile = heads[8 * j : 8 * j + 8]
            tiles += [jnp.where(row8 < 4, tile, 0.0), jnp.where(row8 < 4, 0.0, tile)]
        product = contract_last(jnp.concatenate(tiles, axis=1).astype(BF16), weight)
        return rounded(product[0:4] + product[4:8])

    part = projected(t, wo[pl.ds(half, 32), :]) + projected(1 - t, wox[...])
    stream = tok[...].astype(F32) + part
    line = jnp.concatenate([stream[b : b + 1] for b in range(4)], axis=1)
    sf[pl.ds(dev, 1), :] = line
    spot_f = sf.at[pl.ds(dev, 1), :]
    for p in OTHERS:
        remote(spot_f, spot_f, 7, p).start()
    loads[10].wait()
    loads[11].wait()
    loads[12].wait()
    remote(sf.at[0:127], sf.at[0:127], 7, (0, 1, 0)).wait_recv()

    rows = sf[...]
    squares = jnp.sum(rows * rows, axis=0, keepdims=True)
    group1 = iota((1, 128), 1) // 32
    scale = jnp.zeros((1, 128), F32)
    for b in range(4):
        mine = group1 == b
        whole = jnp.sum(jnp.where(mine, squares, 0.0), axis=1, keepdims=True)
        scale = jnp.where(mine, lax.rsqrt(whole * (1.0 / 4096.0) + EPS), scale)
    normed = rounded(rows * scale * gf[...])
    diagonal = iota((128, 128), 1) // 32 == iota((128, 128), 0) % 4
    lefts = []
    for s in range(4):
        moved = normed if s == 0 else pltpu.roll(normed, 32 * s, 1)
        kept = jnp.where(diagonal, moved, 0.0)
        tiles = []
        for v in range(16):
            tile = kept[8 * v : 8 * v + 8]
            tiles += [jnp.where(row8 < 4, tile, 0.0), jnp.where(row8 < 4, 0.0, tile)]
        lefts.append(jnp.concatenate(tiles, axis=1))
    left = jnp.concatenate(lefts, axis=0).astype(BF16)

    def folded(product):
        result = None
        for s in range(4):
            block = product[8 * s : 8 * s + 8]
            block = block + jnp.concatenate([block[4:8], block[0:4]], axis=0)
            if s:
                block = jnp.concatenate([block[s:8], block[0:s]], axis=0)
            result = block if result is None else result + block
        return result

    gate = folded(contract_last(left, wg[...]))
    up = folded(contract_last(left, wu[...]))
    hidden = gate / (1.0 + jnp.exp(-gate)) * up
    turned = [hidden] + [jnp.concatenate([hidden[s:8], hidden[0:s]], axis=0) for s in range(1, 4)]
    down = jnp.dot(
        jnp.concatenate(turned, axis=0).astype(BF16), wd[...], preferred_element_type=F32
    )
    for v in range(16):
        result = None
        for s in range(4):
            even = down[8 * s : 8 * s + 8, 256 * v : 256 * v + 128]
            odd = down[8 * s : 8 * s + 8, 256 * v + 128 : 256 * v + 256]
            tile = jnp.where(row8 < 4, even, odd)
            if s == 0:
                result = tile
            else:
                place = lane8 // 32 == lax.rem(row8 + s, 4)
                result = jnp.where(place, pltpu.roll(tile, 32 * s, 1), result)
        gs[8 * v : 8 * v + 8, :] = result
    for p in OTHERS:
        _, pz, py, pt = at(*p)
        to = (pz * N + py) * 2 + pt
        remote(gs.at[pl.ds(to, 1), :], gr.at[pl.ds(dev, 1), :], 8, p).start()
    gr[pl.ds(dev, 1), :] = gs[pl.ds(dev, 1), :]
    mine = sf[pl.ds(dev, 1), :]
    remote(gr.at[0:127], gr.at[0:127], 8, (0, 1, 0)).wait_recv()
    out_ref[...] = mine + jnp.sum(gr[...], axis=0, keepdims=True)

    for k, ref in (
        (0, tok), (1, qr), (2, wox), (3, qzr), (4, qa.at[0:7]), (5, sr.at[:, 0:63, :]),
        (6, sf.at[0:127]), (7, sf.at[0:127]), (8, gr.at[0:127]),
    ):
        remote(ref, ref, k, (0, 1, 0)).wait_send()


def rope_tables():
    half = 32
    rate = (1.0 / np.float32(THETA) ** (np.arange(half, dtype=np.float32) / np.float32(half))).astype(np.float32)
    angle = (np.float32(16384) * rate).astype(np.float32).astype(np.float64)
    cos, sin = np.cos(angle).astype(np.float32), np.sin(angle).astype(np.float32)
    table = np.stack([np.tile(cos, 4), np.concatenate([-sin, sin, -sin, sin])])
    return np.ascontiguousarray(np.broadcast_to(table[:, None, :], (2, 8, 128)))


def shards(tokens, attn_gain, query_weight, key_cache, value_cache, head_lambda, head_gain,
           out_weight, mlp_gain, gate_weight, up_weight, down_weight):
    args = (
        tokens, attn_gain.reshape(32, 128), query_weight, key_cache.reshape(4, 256, 128),
        value_cache.reshape(4, 256, 128), head_lambda, head_gain.reshape(1, 128), out_weight,
        mlp_gain.reshape(32, 128), gate_weight, up_weight, down_weight, jnp.asarray(rope_tables()),
    )
    local = [
        pltpu.SMEM(a.shape, a.dtype) if k == 5 else pltpu.VMEM(a.shape, a.dtype)
        for k, a in enumerate(args)
    ]
    wide = lambda *shape: pltpu.VMEM(shape, F32)
    line = pl.pallas_call(
        kernel,
        out_shape=jax.ShapeDtypeStruct((1, 128), F32),
        in_specs=[pl.BlockSpec(memory_space=pl.ANY)] * len(args),
        out_specs=pl.BlockSpec(memory_space=pltpu.VMEM),
        scratch_shapes=local + [
            pltpu.VMEM((4, 32), BF16), pltpu.VMEM((32, 2048), BF16),
            wide(8, 16, 128), wide(7, 16, 128), wide(16, 128), wide(7, 16, 128), wide(8, 8, 128),
            wide(3, 64, 128), wide(3, 64, 128), wide(2, 64, 128), wide(128, 128),
            wide(128, 128), wide(128, 128), wide(128, 128), wide(8, 2048),
            pltpu.SemaphoreType.DMA((13,)), pltpu.SemaphoreType.DMA((1,)),
            pltpu.SemaphoreType.DMA((9,)), pltpu.SemaphoreType.DMA((9,)),
        ],
        compiler_params=pltpu.CompilerParams(collective_id=0, has_side_effects=True),
    )(*args)
    return line.reshape(4, 32).astype(BF16)


def solution(mesh):
    torus = Mesh(mesh.devices.reshape(mesh.shape["dp"], 8, 8, mesh.shape["tp"]), AXES)
    in_specs = (
        P("dp", KV_TP), P(), P(KV, "tp"), P("dp", KV, "tp", None), P("dp", KV, "tp", None),
        P("tp"), P(), P(KV, "tp"), P(), P(KV_TP, None), P(KV_TP, None), P(KV_TP, None),
    )
    return jax.shard_map(
        shards, mesh=torus, in_specs=in_specs, out_specs=P("dp", KV_TP), check_vma=False
    )
```
